32 devices in a mesh: sp: 8 (over z, y), dp: 4 (over x, core).
Axes of the slice: x: 2, y: 2, z: 4, core: 2. Of those that a mesh axis runs over, the one named last changes fastest.
Arguments:
- query_nope: bfloat16 [4, 2048, 16, 128], P('dp', 'sp'), may hold values from -6 to 6
- query_rope: bfloat16 [4, 2048, 16, 64], P('dp', 'sp'), may hold values from -160 to 160
- latent: bfloat16 [4, 2048, 256], P('dp', 'sp'), may hold values from -6 to 6
- key_rope: bfloat16 [4, 2048, 64], P('dp', 'sp'), may hold values from -4 to 4
- resid: bfloat16 [4, 2048, 2048], P('dp', 'sp'), may hold values from -6 to 6
- latent_gain: float32 [256], replicated, may hold values from 0.1 to 1.9
- key_up: bfloat16 [256, 2048], P(None, 'sp'), may hold values from -0.375 to 0.375
- value_up: bfloat16 [256, 2048], P(None, 'sp'), may hold values from -0.375 to 0.375
- out_proj: bfloat16 [2048, 2048], P('sp', 'dp'), may hold values from -0.125 to 0.125
- norm_gain: float32 [2048], replicated, may hold values from 0.1 to 1.9
- expert_gate: bfloat16 [8, 2048, 1024], P('sp'), may hold values from -0.125 to 0.125
- expert_up: bfloat16 [8, 2048, 1024], P('sp'), may hold values from -0.125 to 0.125
- expert_down: bfloat16 [8, 1024, 2048], P('sp'), may hold values from -0.1875 to 0.1875
- routes: int32 [4, 2048, 2], P('dp', 'sp'), may hold values from 0 to 7, all different within a row; in each aligned block of 256 rows (0 to 255, 256 to 511, ..., all dimensions but the last counted through in order) at most 128 rows name the same one
- route_weight: float32 [4, 2048, 2], P('dp', 'sp'), may hold values from 0.2 to 1
Outputs:
- mixed: bfloat16 [4, 2048, 2048], P('dp', 'sp')
The draws below stay inside these ranges and needn't reach their ends.
Inputs may be any that keep to these rules, and one draw needn't show every extreme that they name: `routes`: each token names two different experts. Among the tokens of one device no expert is named more than 128 times, and in every draw some expert is named exactly 128 times by some device's tokens.
All inputs are finite; a program needn't handle non-finite values.
Results may differ from the reference program's by a relative error of at most 0.0075.
Values may be sent and summed in bfloat16 or wider, within the bound.
No kernel may reach another device: no remote copies, remote signals or barrier semaphores. Data moves between devices by JAX's collectives and lax.ppermute only.
A program may use at most 128 MiB of HBM per device.

```python
import math
import jax
import jax.numpy as jnp
import numpy as np
from jax import lax

D = 2048
HEADS = 16
NOPE = 128
ROPE = 64
VDIM = 128
LATENT = 256
FFE = 1024
TOK_DEV = 256
LENGTH = 2048
SEQS = 4
EXPERTS = 8
CAP = 128
N_SP = 8
N_DP = 4


def rope_pair(key):
    base_key = jax.random.fold_in(key, 911)
    key_draw, query_draw = jax.random.split(base_key, 2)
    keys_raw = jnp.clip(jax.random.normal(key_draw, (SEQS, LENGTH, ROPE), jnp.float32), -4.0, 4.0)
    queries = jnp.clip(jax.random.normal(query_draw, (SEQS, LENGTH, HEADS, ROPE), jnp.float32), -4.0, 4.0)
    return (queries, keys_raw)


def draw_query_rope(key, part):
    return rope_pair(key)[0].astype(jnp.bfloat16)


def draw_key_rope(key, part):
    return rope_pair(key)[1].astype(jnp.bfloat16)


def steps_of(rng, extent, cuts, low, top_value):
    def one(axis_at, parts):
        steps = jax.random.uniform(jax.random.fold_in(jax.random.fold_in(rng, 6), axis_at), (parts,), jnp.float32, low / len(cuts), top_value / len(cuts))
        return jnp.repeat(jnp.exp(steps), extent[axis_at] // parts).reshape((-1,) + (1,) * (len(extent) - axis_at - 1))

    factor_of = one(*cuts[0])
    for cut in cuts[1:]:
        factor_of = factor_of * one(*cut)
    return factor_of


def deal_out(key, own, number, rows, count, top, most, lean):
    order = jax.random.permutation(key, count)
    heavy_load, usual = load_shares(count, rows * top, most, lean, True), load_shares(count, rows * top, most, lean, False)
    places = jnp.arange(count)

    def named(tallies, offset_by):
        used = int((tallies > 0).sum())
        fixed = max(1, used // 4)
        shifted = fixed + (places - fixed + offset_by * (used - fixed)) % max(1, count - fixed)
        return jnp.zeros((count,), jnp.int32).at[order[jnp.where(places < fixed, places, shifted)]].set(jnp.asarray(tallies, jnp.int32))

    tallies = jnp.where(number % 4 == 0, named(heavy_load, number // 4), named(usual, number - number // 4 - 1))
    mixed = jax.random.permutation(jax.random.fold_in(own, 3), count)
    giver, receiver = mixed[0:count // 2 * 2:2], mixed[1:count // 2 * 2:2]
    slack = jnp.minimum(tallies[giver] - 1, most - tallies[receiver]) // 2
    slack = jnp.where((giver == order[0]) | (receiver == order[0]) | (tallies[receiver] == 0), 0, jnp.maximum(slack, 0))
    shifted = jax.random.randint(jax.random.fold_in(own, 4), (count // 2,), 0, 1 << 20) % (slack + 1)
    tallies = tallies.at[giver].add(-shifted).at[receiver].add(shifted)
    items = jnp.searchsorted(jnp.cumsum(tallies), jnp.arange(rows * top), side="right").astype(jnp.int32)
    listing = items.reshape(top, rows).T
    listing = listing[jax.random.permutation(jax.random.fold_in(own, 1), rows)]
    offset_by = jax.random.randint(jax.random.fold_in(own, 2), (rows, 1), 0, top)
    return jnp.take_along_axis(listing, (jnp.arange(top)[None, :] + offset_by) % top, axis=1)


def load_shares(number_of, total, limit, slope, full):
    portions = [(1 << 20) // math.isqrt(standing ** slope) + 1 for standing in range(1, number_of + 1)]
    largest = limit if full else min(limit, max(-(-total // number_of), total * portions[0] // sum(portions)))
    least = 1 if total - largest >= number_of - 1 else 0
    counts, rest = [largest] + [least] * (number_of - 1), total - largest - least * (number_of - 1)
    while rest > 0:
        candidates = [i for i in range(1, number_of) if counts[i] < largest] or [i for i in range(1, number_of) if counts[i] < limit]
        mass, remaining = sum([portions[i] for i in candidates]), rest
        for i in candidates:
            more = min(limit - counts[i], max(1, remaining * portions[i] // mass), rest)
            counts[i] = counts[i] + more
            rest = rest - more
    return np.array(counts)


def centred(key, shape, deviation, reach, cuts=(), held_as=jnp.bfloat16):
    drawn = jax.random.normal(key, shape, jnp.float32) * deviation
    if len(cuts) > 0:
        drawn = steps_of(key, shape, cuts, -0.22, 0.18) * drawn
    return jnp.clip(drawn, min=-reach, max=reach).astype(held_as)


def setup_inputs(seed: int = 0) -> dict:
    keys = jax.random.split(jax.random.key(seed), 16)
    query_nope = centred(keys[0], (SEQS, LENGTH, HEADS, NOPE), 1.0, 6.0, ((0, 4), (1, 8)))
    query_rope = draw_query_rope(jax.random.fold_in(keys[15], 71), 0)
    latent = centred(keys[2], (SEQS, LENGTH, LATENT), 1.0, 6.0, ((0, 4), (1, 8)))
    key_rope = draw_key_rope(jax.random.fold_in(keys[15], 71), 0)
    resid = centred(keys[4], (SEQS, LENGTH, D), 1.0, 6.0, ((0, 4), (1, 8)))
    latent_gain = jnp.clip(1.0 + 0.18 * jax.random.normal(keys[5], (LATENT,), jnp.float32), 0.1, 1.9)
    key_up = centred(keys[6], (LATENT, HEADS * NOPE), LATENT ** -0.5, 0.375, ((1, 8),))
    value_up = centred(keys[7], (LATENT, HEADS * VDIM), LATENT ** -0.5, 0.375, ((1, 8),))
    out_proj = centred(keys[8], (HEADS * VDIM, D), (HEADS * VDIM) ** -0.5, 0.125, ((0, 8), (1, 4)))
    norm_gain = jnp.clip(1.0 + 0.18 * jax.random.normal(keys[9], (D,), jnp.float32), 0.1, 1.9)
    expert_gate = centred(keys[10], (EXPERTS, D, FFE), D ** -0.5, 0.125, ((0, 8),))
    expert_up = centred(keys[11], (EXPERTS, D, FFE), D ** -0.5, 0.125, ((0, 8),))
    expert_down = centred(keys[12], (EXPERTS, FFE, D), FFE ** -0.5, 0.1875, ((0, 8),))
    routes_keys = jax.random.split(jax.random.fold_in(keys[13], 1), SEQS * LENGTH // TOK_DEV)
    routes_turns = jax.random.permutation(jax.random.fold_in(keys[13], 3), SEQS * LENGTH // TOK_DEV)
    routes = jax.vmap(lambda own, number: deal_out(jax.random.fold_in(keys[13], 2), own, number, TOK_DEV, EXPERTS, 2, CAP, 1))(routes_keys, routes_turns).reshape((SEQS, LENGTH, 2))
    route_weight = jnp.clip(0.2 + 0.8 * jax.random.uniform(keys[14], (SEQS, LENGTH, 2), jnp.float32) ** steps_of(keys[14], (SEQS, LENGTH, 2), ((0, 4), (1, 8)), -0.2, 0.2), 0.2, 1.0)
    return dict(query_nope=query_nope, query_rope=query_rope, latent=latent, key_rope=key_rope, resid=resid, latent_gain=latent_gain, key_up=key_up, value_up=value_up, out_proj=out_proj, norm_gain=norm_gain, expert_gate=expert_gate, expert_up=expert_up, expert_down=expert_down, routes=routes, route_weight=route_weight)


epsilon = 1e-06
rope_base = 10000.0
masked_score = -1e+30

def rotate(values, positions):
    half_width = values.shape[-1] // 2
    frequency = rope_base ** (-jnp.arange(half_width, dtype=jnp.float32) / half_width)
    angles = positions.astype(jnp.float32)[:, None] * frequency[None, :]
    cosine = jnp.cos(angles)
    sine_part = jnp.sin(angles)
    if values.ndim == 3:
        cosine = cosine[:, None, :]
        sine_part = sine_part[:, None, :]
    floats = values.astype(jnp.float32)
    first_half = floats[..., :half_width]
    second_half = floats[..., half_width:]
    turned = jnp.concatenate([first_half * cosine - second_half * sine_part, second_half * cosine + first_half * sine_part], axis=-1)
    return turned.astype(jnp.bfloat16)

def rms_scaled(values, gain):
    floats = values.astype(jnp.float32)
    return floats * lax.rsqrt(lax.optimization_barrier(jnp.mean(floats * floats, axis=-1, keepdims=True)) + epsilon) * gain

def assign_slots(route_block, experts_all, capacity):
    flat_routes = route_block.reshape(-1)
    onehot = (flat_routes[:, None] == jnp.arange(experts_all, dtype=jnp.int32)[None, :]).astype(jnp.int32)
    earlier = jnp.cumsum(onehot, axis=0) - onehot
    placed = lax.optimization_barrier(jnp.sum(earlier * onehot, axis=1))
    return (flat_routes * capacity + placed).astype(jnp.int32)

def fill_slots(rows, slot_ids, experts_all, capacity):
    pairs = slot_ids.shape[0]
    matches = jnp.arange(experts_all * capacity, dtype=jnp.int32)[:, None] == slot_ids[None, :]
    source = lax.optimization_barrier(jnp.sum(jnp.where(matches, jnp.arange(pairs, dtype=jnp.int32)[None, :], 0), axis=1)) // 2
    filled = jnp.any(matches, axis=1)
    picked = jnp.take(rows, source.astype(jnp.int32), axis=0)
    chosen = jnp.where(filled[:, None], picked, jnp.zeros_like(picked))
    return chosen.reshape(experts_all, capacity, rows.shape[-1])

def combine_slots(returned, slot_ids, weights):
    flat_back = returned.reshape(-1, returned.shape[-1])
    picked = jnp.take(flat_back, slot_ids, axis=0).astype(jnp.float32).reshape(weights.shape[0], 2, -1)
    return lax.optimization_barrier(jnp.sum(weights[:, :, None] * picked, axis=1))

def expert_rows(rows, gate_weight, up_weight, down_weight):
    gate = jnp.dot(rows, gate_weight, preferred_element_type=jnp.float32)
    upward = jnp.dot(rows, up_weight, preferred_element_type=jnp.float32)
    hidden = (jax.nn.silu(gate) * upward).astype(jnp.bfloat16)
    return jnp.dot(hidden, down_weight, preferred_element_type=jnp.float32).astype(jnp.bfloat16)

def head_attention(query_plain, query_turn, key_plain, key_turn, value_head, block):
    length = key_plain.shape[0]
    blocks = length // block
    scale = (query_plain.shape[-1] + query_turn.shape[-1]) ** (-0.5)
    key_ids = jnp.arange(length, dtype=jnp.int32)

    def one_block(items):
        index, plain_block, turn_block = items
        scores = jnp.dot(plain_block, key_plain.T, preferred_element_type=jnp.float32)
        scores = (scores + jnp.dot(turn_block, key_turn.T, preferred_element_type=jnp.float32)) * scale
        row_ids = index * block + jnp.arange(block, dtype=jnp.int32)
        allowed = key_ids[None, :] <= row_ids[:, None]
        scores = jnp.where(allowed, scores, masked_score)
        largest = lax.optimization_barrier(jnp.max(scores, axis=-1, keepdims=True))
        powers = jnp.exp(scores - largest)
        attend = (powers / lax.optimization_barrier(jnp.sum(powers, axis=-1, keepdims=True))).astype(jnp.bfloat16)
        return jnp.dot(attend, value_head, preferred_element_type=jnp.float32).astype(jnp.bfloat16)
    result = lax.map(one_block, (jnp.arange(blocks, dtype=jnp.int32), query_plain.reshape(blocks, block, -1), query_turn.reshape(blocks, block, -1)))
    return result.reshape(length, -1)

def reference(query_nope, query_rope, latent, key_rope, resid, latent_gain, key_up, value_up, out_proj, norm_gain, expert_gate, expert_up, expert_down, routes, route_weight):
    positions = jnp.arange(LENGTH, dtype=jnp.int32)
    block = min(512, LENGTH)
    key_turned = jax.vmap(lambda item: rotate(item, positions))(key_rope)
    query_turned = jax.vmap(lambda item: rotate(item, positions))(query_rope)
    latent_normed = rms_scaled(latent, latent_gain).astype(jnp.bfloat16)
    flat_latent = latent_normed.reshape(-1, LATENT)
    key_nope = jnp.dot(flat_latent, key_up, preferred_element_type=jnp.float32).astype(jnp.bfloat16).reshape(SEQS, LENGTH, HEADS, NOPE)
    values = jnp.dot(flat_latent, value_up, preferred_element_type=jnp.float32).astype(jnp.bfloat16).reshape(SEQS, LENGTH, HEADS, VDIM)

    def one_sequence(items):
        plain_heads, turn_heads, key_heads, value_heads, key_turn = items
        return lax.map(lambda head: head_attention(head[0], head[1], head[2], key_turn, head[3], block), (plain_heads, turn_heads, key_heads, value_heads))
    heads_out = lax.map(one_sequence, (jnp.transpose(query_nope, (0, 2, 1, 3)), jnp.transpose(query_turned, (0, 2, 1, 3)), jnp.transpose(key_nope, (0, 2, 1, 3)), jnp.transpose(values, (0, 2, 1, 3)), key_turned))
    heads_out = jnp.transpose(heads_out, (0, 2, 1, 3)).reshape(SEQS * LENGTH, HEADS * VDIM)
    projected = jnp.dot(heads_out, out_proj, preferred_element_type=jnp.float32).astype(jnp.bfloat16)
    after_attention = resid.reshape(-1, D).astype(jnp.float32) + projected.astype(jnp.float32)
    normed = rms_scaled(after_attention, norm_gain).astype(jnp.bfloat16)
    normed_blocks = normed.reshape(N_DP, N_SP, TOK_DEV, D)
    route_blocks = routes.reshape(N_DP, N_SP, TOK_DEV, 2)
    slot_ids = jax.vmap(jax.vmap(lambda item: assign_slots(item, EXPERTS, CAP)))(route_blocks)
    buffers = jax.vmap(jax.vmap(lambda rows, ids: fill_slots(rows, ids, EXPERTS, CAP)))(normed_blocks, slot_ids)
    by_expert = jnp.transpose(buffers, (2, 0, 1, 3, 4)).reshape(EXPERTS, N_DP * N_SP * CAP, D)
    outputs = lax.map(lambda item: expert_rows(item[0], item[1], item[2], item[3]), (by_expert, expert_gate, expert_up, expert_down))
    returned = jnp.transpose(outputs.reshape(EXPERTS, N_DP, N_SP, CAP, D), (1, 2, 0, 3, 4))
    routed = jax.vmap(jax.vmap(combine_slots))(returned, slot_ids, route_weight.reshape(N_DP, N_SP, TOK_DEV, 2))
    mixed = after_attention + routed.reshape(-1, D)
    return mixed.astype(jnp.bfloat16).reshape(SEQS, LENGTH, D)
```

```python
import jax
import jax.numpy as jnp
from jax import lax
from jax.experimental import pallas as pl
from jax.experimental.pallas import tpu as pltpu
from jax.sharding import PartitionSpec as P

epsilon = 1e-06
rope_base = 10000.0
masked_score = -1e30


def rotate(values, positions):
    half_width = values.shape[-1] // 2
    frequency = rope_base ** (-jnp.arange(half_width, dtype=jnp.float32) / half_width)
    angles = positions.astype(jnp.float32)[:, None] * frequency[None, :]
    cosine = jnp.cos(angles)
    sine_part = jnp.sin(angles)
    if values.ndim == 3:
        cosine = cosine[:, None, :]
        sine_part = sine_part[:, None, :]
    floats = values.astype(jnp.float32)
    first_half = floats[..., :half_width]
    second_half = floats[..., half_width:]
    turned = jnp.concatenate(
        [
            first_half * cosine - second_half * sine_part,
            second_half * cosine + first_half * sine_part,
        ],
        axis=-1,
    )
    return turned.astype(jnp.bfloat16)


def rms_scaled(values, gain):
    floats = values.astype(jnp.float32)
    return floats * lax.rsqrt(jnp.mean(floats * floats, axis=-1, keepdims=True) + epsilon) * gain


def assign_slots(route_block, experts_all, capacity):
    flat_routes = route_block.reshape(-1)
    onehot = (flat_routes[:, None] == jnp.arange(experts_all, dtype=jnp.int32)[None, :]).astype(
        jnp.int32
    )
    earlier = jnp.cumsum(onehot, axis=0) - onehot
    placed = jnp.sum(earlier * onehot, axis=1)
    return flat_routes * capacity + placed


def one_hot_slots(slot_ids, slots):
    ids = jnp.arange(slots, dtype=jnp.int32)
    return (slot_ids[:, None] == ids[None, :]).astype(jnp.bfloat16)


def attention_kernel(
    heads, nope, block, scale, query_ref, latent_ref, tail_ref, key_up_ref, value_up_ref, out_ref
):
    length = query_ref.shape[0]
    value_width = value_up_ref.shape[1] // heads
    factor = scale * 1.4426950408889634
    keys = jnp.dot(
        latent_ref[...], key_up_ref[...], preferred_element_type=jnp.float32
    ).astype(jnp.bfloat16)
    values = jnp.dot(
        latent_ref[...], value_up_ref[...], preferred_element_type=jnp.float32
    ).astype(jnp.bfloat16)
    rows = lax.broadcasted_iota(jnp.int32, (block, block), 0)
    columns = lax.broadcasted_iota(jnp.int32, (block, block), 1)
    allowed = columns <= rows
    contract_last = (((1,), (1,)), ((), ()))
    for step in range(length // block):
        low = step * block
        high = low + block
        turned = query_ref[low:high, heads * nope :]
        for head in range(heads):
            full_keys = jnp.concatenate(
                [keys[:high, head * nope : (head + 1) * nope], tail_ref[head, :high, :]], axis=1
            )
            full_query = jnp.concatenate(
                [query_ref[low:high, head * nope : (head + 1) * nope], turned], axis=1
            )
            scores = lax.dot_general(
                full_query, full_keys, contract_last, preferred_element_type=jnp.float32
            )
            own = jnp.where(allowed, scores[:, low:], masked_score)
            if step:
                scores = jnp.concatenate([scores[:, :low], own], axis=1)
            else:
                scores = own
            largest = jnp.max(scores, axis=-1, keepdims=True)
            powers = jnp.exp2((scores - largest) * factor)
            total = jnp.sum(powers, axis=-1, keepdims=True)
            picked = jnp.dot(
                powers.astype(jnp.bfloat16),
                values[:high, head * value_width : (head + 1) * value_width],
                preferred_element_type=jnp.float32,
            )
            out_ref[low:high, head * value_width : (head + 1) * value_width] = (
                picked / total
            ).astype(jnp.bfloat16)


def attention(queries, latents, tails, key_up, value_up, nope, block, scale):
    heads = tails.shape[0]
    return pl.pallas_call(
        lambda *refs: attention_kernel(heads, nope, block, scale, *refs),
        out_shape=jax.ShapeDtypeStruct((queries.shape[0], value_up.shape[1]), jnp.bfloat16),
        in_specs=[pl.BlockSpec(memory_space=pltpu.VMEM)] * 5,
        out_specs=pl.BlockSpec(memory_space=pltpu.VMEM),
        compiler_params=pltpu.CompilerParams(vmem_limit_bytes=56 * 1024 * 1024),
    )(queries, latents, tails, key_up, value_up)


def shards(
    query_nope,
    query_rope,
    latent,
    key_rope,
    resid,
    latent_gain,
    key_up,
    value_up,
    out_proj,
    norm_gain,
    expert_gate,
    expert_up,
    expert_down,
    routes,
    route_weight,
):
    tokens_here = latent.shape[1]
    sp_count = lax.axis_size("sp")
    length = tokens_here * sp_count
    heads_all, nope = query_nope.shape[2:]
    turn = query_rope.shape[3]
    heads_here = heads_all // sp_count
    latent_width = latent.shape[2]
    local_pos = lax.axis_index("sp") * tokens_here + jnp.arange(tokens_here, dtype=jnp.int32)
    latent_normed = rms_scaled(latent[0], latent_gain).astype(jnp.bfloat16)
    key_turned = rotate(key_rope[0], local_pos)
    query_turned = rotate(query_rope[0], local_pos)
    all_proj = lax.all_gather(out_proj, ("sp", "dp"))
    cut = latent_width - turn
    first_part = lax.all_gather(latent_normed[:, :cut], "sp", axis=0, tiled=True)
    second_part = lax.all_gather(
        jnp.concatenate([latent_normed[:, cut:], key_turned], axis=1), "sp", axis=0, tiled=True
    )
    all_latent = jnp.concatenate([first_part, second_part[:, :turn]], axis=1)
    all_keyturn = second_part[:, turn:]
    packed_query = jnp.concatenate(
        [
            query_nope[0].reshape(tokens_here, sp_count, heads_here * nope),
            query_turned.reshape(tokens_here, sp_count, heads_here * turn),
        ],
        axis=2,
    ).transpose(1, 0, 2)
    queries = lax.all_to_all(packed_query, "sp", split_axis=0, concat_axis=0, tiled=True)
    queries = queries.reshape(length, -1)
    tails = jnp.stack(
        [
            jnp.pad(all_keyturn, ((0, 0), (head * turn, (heads_here - 1 - head) * turn)))
            for head in range(heads_here)
        ]
    )
    attended = attention(
        queries, all_latent, tails, key_up, value_up, nope, min(256, length), (nope + turn) ** (-0.5)
    )
    token_heads = lax.all_to_all(
        attended.reshape(sp_count, tokens_here, -1), "sp", split_axis=0, concat_axis=0, tiled=True
    )
    dp_count = lax.axis_size("dp")
    all_proj = all_proj.reshape(sp_count, dp_count, out_proj.shape[0], out_proj.shape[1])
    projected = jnp.einsum(
        "stk,sdkn->tdn", token_heads, all_proj, preferred_element_type=jnp.float32
    ).astype(jnp.bfloat16).reshape(tokens_here, -1)
    after_attention = resid[0].astype(jnp.float32) + projected.astype(jnp.float32)
    normed = rms_scaled(after_attention, norm_gain).astype(jnp.bfloat16)
    experts_all = sp_count * expert_gate.shape[0]
    capacity = 4 * tokens_here // experts_all
    slot_ids = assign_slots(routes[0], experts_all, capacity).reshape(tokens_here, 2)
    slots = experts_all * capacity
    first_slots = one_hot_slots(slot_ids[:, 0], slots)
    second_slots = one_hot_slots(slot_ids[:, 1], slots)
    outgoing = lax.dot_general(
        first_slots + second_slots,
        normed,
        (((0,), (0,)), ((), ())),
        preferred_element_type=jnp.float32,
    ).astype(jnp.bfloat16)
    arrived = lax.all_to_all(
        outgoing.reshape(experts_all, capacity, -1), "sp", split_axis=0, concat_axis=0, tiled=True
    )
    senders, slots_now, width = arrived.shape
    rows = arrived.reshape(senders * slots_now, width)
    gate = jnp.dot(rows, expert_gate[0], preferred_element_type=jnp.float32)
    upward = jnp.dot(rows, expert_up[0], preferred_element_type=jnp.float32)
    hidden = (jax.nn.silu(gate) * upward).astype(jnp.bfloat16)
    result = jnp.dot(hidden, expert_down[0], preferred_element_type=jnp.float32).astype(
        jnp.bfloat16
    )
    returned = lax.all_to_all(
        result.reshape(senders, slots_now, width), "sp", split_axis=0, concat_axis=0, tiled=True
    ).reshape(slots, width)
    weights = route_weight[0]
    routed = weights[:, :1] * jnp.dot(
        first_slots, returned, preferred_element_type=jnp.float32
    ) + weights[:, 1:] * jnp.dot(second_slots, returned, preferred_element_type=jnp.float32)
    return (after_attention + routed).astype(jnp.bfloat16)[None]


def solution(mesh):
    return jax.shard_map(
        shards,
        mesh=mesh,
        in_specs=(
            P("dp", "sp", None, None),
            P("dp", "sp", None, None),
            P("dp", "sp", None),
            P("dp", "sp", None),
            P("dp", "sp", None),
            P(),
            P(None, "sp"),
            P(None, "sp"),
            P("sp", "dp"),
            P(),
            P("sp", None, None),
            P("sp", None, None),
            P("sp", None, None),
            P("dp", "sp", None),
            P("dp", "sp", None),
        ),
        out_specs=P("dp", "sp", None),
        check_vma=False,
    )
```

```python
import jax
import jax.numpy as jnp
from jax import lax
from jax.experimental import pallas as pl
from jax.experimental.pallas import tpu as pltpu
from jax.sharding import PartitionSpec as P

epsilon = 1e-06
rope_base = 10000.0
masked_score = -1e30


def rotate(values, positions):
    half_width = values.shape[-1] // 2
    frequency = rope_base ** (-jnp.arange(half_width, dtype=jnp.float32) / half_width)
    angles = positions.astype(jnp.float32)[:, None] * frequency[None, :]
    cosine = jnp.cos(angles)
    sine_part = jnp.sin(angles)
    if values.ndim == 3:
        cosine = cosine[:, None, :]
        sine_part = sine_part[:, None, :]
    floats = values.astype(jnp.float32)
    first_half = floats[..., :half_width]
    second_half = floats[..., half_width:]
    turned = jnp.concatenate(
        [
            first_half * cosine - second_half * sine_part,
            second_half * cosine + first_half * sine_part,
        ],
        axis=-1,
    )
    return turned.astype(jnp.bfloat16)


def rms_scaled(values, gain):
    floats = values.astype(jnp.float32)
    return floats * lax.rsqrt(jnp.mean(floats * floats, axis=-1, keepdims=True) + epsilon) * gain


def assign_slots(route_block, experts_all, capacity):
    flat_routes = route_block.reshape(-1)
    onehot = (flat_routes[:, None] == jnp.arange(experts_all, dtype=jnp.int32)[None, :]).astype(
        jnp.int32
    )
    earlier = jnp.cumsum(onehot, axis=0) - onehot
    placed = jnp.sum(earlier * onehot, axis=1)
    return flat_routes * capacity + placed


def one_hot_slots(slot_ids, slots):
    ids = jnp.arange(slots, dtype=jnp.int32)
    return (slot_ids[:, None] == ids[None, :]).astype(jnp.bfloat16)


def ring_gather(local):
    count = lax.axis_size("sp")
    order = list(range(0, count, 2)) + list(range(count - 1, 0, -2))
    onward = [(order[i], order[(i + 1) % count]) for i in range(count)]
    backward = [(target, source) for source, target in onward]
    place = jnp.array([order.index(i) for i in range(count)])[lax.axis_index("sp")]
    blocks = [local]
    offsets = [0]
    ahead = behind = local
    for step in range(1, count // 2 + 1):
        ahead = lax.ppermute(ahead, "sp", onward)
        blocks.append(ahead)
        offsets.append(-step)
        if step <= (count - 1) // 2:
            behind = lax.ppermute(behind, "sp", backward)
            blocks.append(behind)
            offsets.append(step)
    sources = jnp.array(order)[(place + jnp.array(offsets)) % count]
    return blocks, sources.astype(jnp.int32)


def column_gather(local):
    count = lax.axis_size("dp")
    here = lax.axis_index("dp")
    across = [(i, (i + 2) % count) for i in range(count)]
    swap = [(i, i ^ 1) for i in range(count)]
    pieces = [local]
    sources = [here]
    current = local
    for step in range(1, count // 2):
        current = lax.ppermute(current, "dp", across)
        pieces.append(current)
        sources.append((here - 2 * step) % count)
    for step in range(count // 2):
        pieces.append(lax.ppermute(pieces[step], "dp", swap))
        sources.append(((here ^ 1) - 2 * step) % count)
    return pieces, jnp.stack(sources).astype(jnp.int32)


def projection_kernel(count, sources_ref, columns_ref, heads_ref, *refs):
    pieces, out_ref = refs[:-1], refs[-1]
    width = pieces[0].shape[2]
    heads = [heads_ref[sources_ref[step]] for step in range(count)]
    for index, piece in enumerate(pieces):
        total = jnp.dot(heads[0], piece[0], preferred_element_type=jnp.float32)
        for step in range(1, count):
            total += jnp.dot(heads[step], piece[step], preferred_element_type=jnp.float32)
        start = pl.multiple_of(columns_ref[index] * width, width)
        out_ref[:, pl.ds(start, width)] = total.astype(jnp.bfloat16)


def project(sources, columns, token_heads, pieces):
    count, rows, _ = token_heads.shape
    width = len(pieces) * pieces[0].shape[2]
    return pl.pallas_call(
        lambda *refs: projection_kernel(count, *refs),
        out_shape=jax.ShapeDtypeStruct((rows, width), jnp.bfloat16),
        in_specs=[pl.BlockSpec(memory_space=pltpu.SMEM)] * 2
        + [pl.BlockSpec(memory_space=pltpu.VMEM)] * (1 + len(pieces)),
        out_specs=pl.BlockSpec(memory_space=pltpu.VMEM),
        compiler_params=pltpu.CompilerParams(vmem_limit_bytes=48 * 1024 * 1024),
    )(sources, columns, token_heads, *pieces)


def attention_kernel(heads, nope, block, scale, count, *refs):
    sources_ref, query_ref, key_up_ref, value_up_ref = refs[:4]
    latent_refs = refs[4 : 4 + count]
    out_ref, keys, values, tail_ref = refs[4 + count :]
    length = query_ref.shape[0]
    value_width = value_up_ref.shape[1] // heads
    factor = scale * 1.4426950408889634
    latent_width = key_up_ref.shape[0]
    for step in range(count):
        tokens, packed_width = latent_refs[step].shape
        turn = packed_width - latent_width
        start = pl.multiple_of(sources_ref[step] * tokens, tokens)
        latent = latent_refs[step][:, :latent_width]
        key_turn = latent_refs[step][:, latent_width:]
        keys[pl.ds(start, tokens), :] = jnp.dot(
            latent, key_up_ref[...], preferred_element_type=jnp.float32
        ).astype(jnp.bfloat16)
        values[pl.ds(start, tokens), :] = jnp.dot(
            latent, value_up_ref[...], preferred_element_type=jnp.float32
        ).astype(jnp.bfloat16)
        blank = jnp.zeros((tokens, turn), jnp.bfloat16)
        for head in range(heads):
            tail_ref[head, pl.ds(start, tokens), :] = jnp.concatenate(
                [key_turn if other == head else blank for other in range(heads)], axis=1
            )
    rows = lax.broadcasted_iota(jnp.int32, (block, block), 0)
    columns = lax.broadcasted_iota(jnp.int32, (block, block), 1)
    allowed = columns <= rows
    contract_last = (((1,), (1,)), ((), ()))
    for step in range(length // block):
        low = step * block
        high = low + block
        turned = query_ref[low:high, heads * nope :]
        for head in range(heads):
            full_keys = jnp.concatenate(
                [keys[:high, head * nope : (head + 1) * nope], tail_ref[head, :high, :]], axis=1
            )
            full_query = jnp.concatenate(
                [query_ref[low:high, head * nope : (head + 1) * nope], turned], axis=1
            )
            scores = lax.dot_general(
                full_query, full_keys, contract_last, preferred_element_type=jnp.float32
            )
            own = jnp.where(allowed, scores[:, low:], masked_score)
            if step:
                scores = jnp.concatenate([scores[:, :low], own], axis=1)
            else:
                scores = own
            largest = jnp.max(scores, axis=-1, keepdims=True)
            powers = jnp.exp2((scores - largest) * factor)
            total = jnp.sum(powers, axis=-1, keepdims=True)
            picked = jnp.dot(
                powers.astype(jnp.bfloat16),
                values[:high, head * value_width : (head + 1) * value_width],
                preferred_element_type=jnp.float32,
            )
            out_ref[low:high, head * value_width : (head + 1) * value_width] = (
                picked / total
            ).astype(jnp.bfloat16)


def attention(sources, queries, blocks, key_up, value_up, heads, nope, block, scale):
    length, packed_width = queries.shape
    count = len(blocks)
    return pl.pallas_call(
        lambda *refs: attention_kernel(heads, nope, block, scale, count, *refs),
        out_shape=jax.ShapeDtypeStruct((length, value_up.shape[1]), jnp.bfloat16),
        in_specs=[pl.BlockSpec(memory_space=pltpu.SMEM)]
        + [pl.BlockSpec(memory_space=pltpu.VMEM)] * (3 + count),
        out_specs=pl.BlockSpec(memory_space=pltpu.VMEM),
        scratch_shapes=[
            pltpu.VMEM((length, key_up.shape[1]), jnp.bfloat16),
            pltpu.VMEM((length, value_up.shape[1]), jnp.bfloat16),
            pltpu.VMEM((heads, length, packed_width - heads * nope), jnp.bfloat16),
        ],
        compiler_params=pltpu.CompilerParams(vmem_limit_bytes=56 * 1024 * 1024),
    )(sources, queries, key_up, value_up, *blocks)


def shards(
    query_nope,
    query_rope,
    latent,
    key_rope,
    resid,
    latent_gain,
    key_up,
    value_up,
    out_proj,
    norm_gain,
    expert_gate,
    expert_up,
    expert_down,
    routes,
    route_weight,
):
    tokens_here = latent.shape[1]
    sp_count = lax.axis_size("sp")
    length = tokens_here * sp_count
    heads_all, nope = query_nope.shape[2:]
    turn = query_rope.shape[3]
    heads_here = heads_all // sp_count
    local_pos = lax.axis_index("sp") * tokens_here + jnp.arange(tokens_here, dtype=jnp.int32)
    latent_normed = rms_scaled(latent[0], latent_gain).astype(jnp.bfloat16)
    key_turned = rotate(key_rope[0], local_pos)
    query_turned = rotate(query_rope[0], local_pos)
    latent_blocks, sources = ring_gather(jnp.concatenate([latent_normed, key_turned], axis=1))
    row_blocks, _ = ring_gather(out_proj)
    pieces, columns = column_gather(jnp.stack(row_blocks))
    packed_query = jnp.concatenate(
        [
            query_nope[0].reshape(tokens_here, sp_count, heads_here * nope),
            query_turned.reshape(tokens_here, sp_count, heads_here * turn),
        ],
        axis=2,
    ).transpose(1, 0, 2)
    queries = lax.all_to_all(packed_query, "sp", split_axis=0, concat_axis=0, tiled=True)
    queries = queries.reshape(length, -1)
    attended = attention(
        sources,
        queries,
        latent_blocks,
        key_up,
        value_up,
        heads_here,
        nope,
        min(256, length),
        (nope + turn) ** (-0.5),
    )
    token_heads = lax.all_to_all(
        attended.reshape(sp_count, tokens_here, -1), "sp", split_axis=0, concat_axis=0, tiled=True
    )
    projected = project(sources, columns, token_heads, pieces)
    after_attention = resid[0].astype(jnp.float32) + projected.astype(jnp.float32)
    normed = rms_scaled(after_attention, norm_gain).astype(jnp.bfloat16)
    experts_all = sp_count * expert_gate.shape[0]
    capacity = 4 * tokens_here // experts_all
    slot_ids = assign_slots(routes[0], experts_all, capacity).reshape(tokens_here, 2)
    slots = experts_all * capacity
    first_slots = one_hot_slots(slot_ids[:, 0], slots)
    second_slots = one_hot_slots(slot_ids[:, 1], slots)
    outgoing = lax.dot_general(
        first_slots + second_slots,
        normed,
        (((0,), (0,)), ((), ())),
        preferred_element_type=jnp.float32,
    ).astype(jnp.bfloat16)
    arrived = lax.all_to_all(
        outgoing.reshape(experts_all, capacity, -1), "sp", split_axis=0, concat_axis=0, tiled=True
    )
    senders, slots_now, width = arrived.shape
    rows = arrived.reshape(senders * slots_now, width)
    gate = jnp.dot(rows, expert_gate[0], preferred_element_type=jnp.float32)
    upward = jnp.dot(rows, expert_up[0], preferred_element_type=jnp.float32)
    hidden = (jax.nn.silu(gate) * upward).astype(jnp.bfloat16)
    result = jnp.dot(hidden, expert_down[0], preferred_element_type=jnp.float32).astype(
        jnp.bfloat16
    )
    returned = lax.all_to_all(
        result.reshape(senders, slots_now, width), "sp", split_axis=0, concat_axis=0, tiled=True
    ).reshape(slots, width)
    weights = route_weight[0]
    routed = weights[:, :1] * jnp.dot(
        first_slots, returned, preferred_element_type=jnp.float32
    ) + weights[:, 1:] * jnp.dot(second_slots, returned, preferred_element_type=jnp.float32)
    return (after_attention + routed).astype(jnp.bfloat16)[None]


def solution(mesh):
    return jax.shard_map(
        shards,
        mesh=mesh,
        in_specs=(
            P("dp", "sp", None, None),
            P("dp", "sp", None, None),
            P("dp", "sp", None),
            P("dp", "sp", None),
            P("dp", "sp", None),
            P(),
            P(None, "sp"),
            P(None, "sp"),
            P("sp", "dp"),
            P(),
            P("sp", None, None),
            P("sp", None, None),
            P("sp", None, None),
            P("dp", "sp", None),
            P("dp", "sp", None),
        ),
        out_specs=P("dp", "sp", None),
        check_vma=False,
    )
```
